32 devices in a mesh: grp: 2 (over y), ra: 4 (over z), cb: 4 (over x, core).
Axes of the slice: x: 2, y: 2, z: 4, core: 2. Of those that a mesh axis runs over, the one named last changes fastest.
Arguments:
- stream: bfloat16 [256, 4096], P('grp', 'ra'), parts along dimension 0, may hold values from -180 to 180
- w_gate: float32 [2, 4096, 11264], P(None, 'ra', 'cb'), may hold values from -0.09375 to 0.09375
- w_up: float32 [2, 4096, 11264], P(None, 'ra', 'cb'), may hold values from -0.09375 to 0.09375
- w_down: float32 [2, 11264, 4096], P(None, 'cb', 'ra'), may hold values from -0.0546875 to 0.0546875
- gate_scale: float32 [2, 11264], P(None, 'cb'), may hold values from 0.5 to 2
- up_scale: float32 [2, 11264], P(None, 'cb'), may hold values from 0.5 to 2
- down_scale: float32 [2, 4096], P(None, 'ra'), may hold values from 0.5 to 2
- pre_gain: float32 [2, 4096], P(None, 'ra'), may hold values from 0.1 to 1.9
- out_gain: float32 [4096], P('ra'), may hold values from 0.1 to 1.9
Outputs:
- normed: bfloat16 [256, 4096], P('grp', 'ra'), parts along dimension 0
The draws below stay inside these ranges and needn't reach their ends.
There are 2 independent parts, one for each index of `grp`. The reference program is written for one: setup_inputs(seed, part) draws one part's arguments, and reference() takes and returns one part's arrays. A program takes and returns all parts, laid end to end along the dimension named above; an argument that names none is the same for every part. Nothing has to cross between parts.
All inputs are finite; a program needn't handle non-finite values.
Results may differ from the reference program's by a relative error of at most 0.018.
Values may be sent and summed in bfloat16 or wider, within the bound.
A program may use at most 192 MiB of HBM per device.

```python
import math
import jax
import jax.numpy as jnp
from jax import lax

D = 4096
FF = 11264
LAYERS = 2
TOK = 128
N_CB = 4


def draw_stream(key, part):
    first = jax.random.fold_in(key, 11)
    second = jax.random.fold_in(key, 12)
    channel = jnp.exp(math.log(3.0) * jnp.arange(D, dtype=jnp.float32) / D)
    base = jnp.clip(jax.random.normal(first, (TOK, D), jnp.float32), -6.0, 6.0)
    rows = jnp.exp(jax.random.uniform(second, (TOK, 1), jnp.float32, 0.0, math.log(10.0)))
    return (base * rows * channel[None, :]).astype(jnp.bfloat16)


def shard_levels(key, extent, split, least, top_value):
    def one(axis_at, blocks):
        heights = jax.random.uniform(jax.random.fold_in(jax.random.fold_in(key, 6), axis_at), (blocks,), jnp.float32, least / len(split), top_value / len(split))
        return jnp.repeat(jnp.exp(heights), extent[axis_at] // blocks).reshape((-1,) + (1,) * (len(extent) - axis_at - 1))

    factor_of = one(*split[0])
    for cut in split[1:]:
        factor_of = factor_of * one(*cut)
    return factor_of


def gaussian(rng, extent, width, most, cuts=(), held_as=jnp.bfloat16):
    level = shard_levels(rng, extent, cuts, -0.22, 0.18) if cuts else 1.0
    array = jax.random.normal(rng, extent, jnp.float32) * width * level
    return jnp.minimum(jnp.maximum(array, -most), most).astype(held_as)


def setup_inputs(seed: int = 0, part: int = 0) -> dict:
    splits = jax.random.split(jax.random.key(seed), 10)
    part_splits = jax.random.split(jax.random.fold_in(splits[9], part), 10)
    stream = draw_stream(jax.random.fold_in(jax.random.fold_in(splits[9], part), 71), part)
    w_gate = gaussian(splits[1], (LAYERS, D, FF), D ** -0.5, 0.09375, ((1, 4), (2, 4)), jnp.float32)
    w_up = gaussian(splits[2], (LAYERS, D, FF), D ** -0.5, 0.09375, ((1, 4), (2, 4)), jnp.float32)
    w_down = gaussian(splits[3], (LAYERS, FF, D), FF ** -0.5, 0.0546875, ((1, 4), (2, 4)), jnp.float32)
    gate_scale = jnp.clip(jnp.exp(math.log(2.0) - 1.3862944 * jax.random.uniform(splits[4], (LAYERS, FF), jnp.float32) ** shard_levels(splits[4], (LAYERS, FF), ((1, 4),), -0.2, 0.2)), 0.5, 2.0)
    up_scale = jnp.clip(jnp.exp(math.log(2.0) - 1.3862944 * jax.random.uniform(splits[5], (LAYERS, FF), jnp.float32) ** shard_levels(splits[5], (LAYERS, FF), ((1, 4),), -0.2, 0.2)), 0.5, 2.0)
    down_scale = jnp.clip(jnp.exp(math.log(2.0) - 1.3862944 * jax.random.uniform(splits[6], (LAYERS, D), jnp.float32) ** shard_levels(splits[6], (LAYERS, D), ((1, 4),), -0.2, 0.2)), 0.5, 2.0)
    pre_gain = jnp.clip(1.0 + 0.18 * jax.random.normal(splits[7], (LAYERS, D), jnp.float32), 0.1, 1.9)
    out_gain = jnp.clip(1.0 + 0.18 * jax.random.normal(splits[8], (D,), jnp.float32), 0.1, 1.9)
    return dict(stream=stream, w_gate=w_gate, w_up=w_up, w_down=w_down, gate_scale=gate_scale, up_scale=up_scale, down_scale=down_scale, pre_gain=pre_gain, out_gain=out_gain)


def reference(stream, w_gate, w_up, w_down, gate_scale, up_scale, down_scale, pre_gain, out_gain):
    current = stream
    for layer in range(LAYERS):
        xvals = lax.optimization_barrier(current).astype(jnp.float32)
        rinv = lax.rsqrt(lax.optimization_barrier(jnp.mean(xvals * xvals, axis=1, keepdims=True)) + 1e-06)
        scaled = (xvals * pre_gain[layer]).astype(jnp.bfloat16)
        gate = jnp.dot(scaled, w_gate[layer].astype(jnp.bfloat16), preferred_element_type=jnp.float32) * rinv * gate_scale[layer]
        upper = jnp.dot(scaled, w_up[layer].astype(jnp.bfloat16), preferred_element_type=jnp.float32) * rinv * up_scale[layer]
        hidden = (jax.nn.silu(gate) * upper).astype(jnp.bfloat16)
        blocks = hidden.astype(jnp.float32).reshape(TOK, N_CB, FF // N_CB)
        down_blocks = w_down[layer].astype(jnp.bfloat16).astype(jnp.float32).reshape(N_CB, FF // N_CB, D)
        partial_value = jnp.einsum('tcf,cfd->ctd', blocks, down_blocks).astype(jnp.bfloat16)
        branch = lax.optimization_barrier(jnp.sum(partial_value.astype(jnp.float32), axis=0)) * down_scale[layer]
        current = (0.5 * xvals + branch).astype(jnp.bfloat16)
    xvals = lax.optimization_barrier(current).astype(jnp.float32)
    rinv = lax.rsqrt(lax.optimization_barrier(jnp.mean(xvals * xvals, axis=1, keepdims=True)) + 1e-06)
    return (xvals * rinv * out_gain).astype(jnp.bfloat16)
```

```python
import functools

import jax
import jax.numpy as jnp
from jax import lax
from jax.experimental import pallas as pl
from jax.experimental.pallas import tpu as pltpu
from jax.sharding import PartitionSpec as P

F32, BF16 = jnp.float32, jnp.bfloat16
MESH = pl.DeviceIdType.MESH
EPS = 1e-06
WIDTH = 128
PAIR = 2
GROUPS = 2
LAG = 5
ENDS = (0, 0, 0, 0)
AFTER = (2, 5, 2, 5)
UP_SLOTS = 8
DOWN_SLOTS = 8
LANES = 128


def plan(n, layers, chunks):
    phases = layers * GROUPS
    ends = [min(ENDS[s % len(ENDS)], chunks) for s in range(phases)]
    start, ready = [], []
    for s in range(phases):
        at = start[s - 1] + chunks if s else 0
        if s >= GROUPS:
            at = max(at, ready[s - GROUPS] + sum(AFTER[:3]))
        start.append(at)
        last = at + chunks - 1 + (n - 1) * LAG if ends[s] < chunks else 0
        if ends[s]:
            last = max(last, at + ends[s] - 1 + 2 * (n - 1) * LAG)
        ready.append(last)
    return ends, start, ready


def body(n, layers, dim, chunks, stream, wg, wu, wd, gs, us, ds, pg, og, out,
         ust, dst, wub, wdb, usem, dsem, xb, scaled, own, sr, sl, gr, gl, hid, acc, rinv_ref, scales, ss,
         c1s, c1r, c2s, c2r, rsend, rrecv, lsend, lrecv, hsend, hrecv, sss, rss, cs, cr):
    p = lax.axis_index("ra")
    q = lax.axis_index("cb")
    core = lax.rem(q, 2)
    mate = q + 1 - 2 * core
    xmate = lax.rem(q + 2, 4)
    w = WIDTH
    rows = stream.shape[0] // GROUPS
    half = rows // 2
    phases = layers * GROUPS
    blocks = chunks // PAIR
    total = layers * blocks
    wide = PAIR * w
    ring = own.shape[0]
    ends, start, ready = plan(n, layers, chunks)
    everything, low, high = slice(0, rows), slice(0, half), slice(half, rows)

    def up_copies(v):
        l, b, k = v // blocks, lax.rem(v, blocks), lax.rem(v, UP_SLOTS)
        at = pl.ds(pl.multiple_of(b * wide, wide), wide)
        return (pltpu.make_async_copy(wg.at[l, :, at], ust.at[k, 0], usem.at[k, 0]),
                pltpu.make_async_copy(wu.at[l, :, at], ust.at[k, 1], usem.at[k, 1]))

    def down_copy(v):
        l, b, k = v // blocks, lax.rem(v, blocks), lax.rem(v, DOWN_SLOTS)
        at = pl.ds(pl.multiple_of(b * wide, wide), wide)
        return pltpu.make_async_copy(wd.at[l, at, :], dst.at[k], dsem.at[k])

    for v in range(min(max(UP_SLOTS, DOWN_SLOTS), total)):
        if v < UP_SLOTS:
            for copy in up_copies(v):
                copy.start()
        if v < DOWN_SLOTS:
            down_copy(v).start()

    barrier = pltpu.get_barrier_semaphore()
    for k in range(1, n):
        pl.semaphore_signal(barrier, inc=1, device_id={"ra": lax.rem(p + k, n)}, device_id_type=MESH)
    pl.semaphore_signal(barrier, inc=1, device_id={"cb": mate}, device_id_type=MESH)
    pl.semaphore_signal(barrier, inc=1, device_id={"cb": xmate}, device_id_type=MESH)

    def remote(src, dst, send, recv, **where):
        return pltpu.make_async_remote_copy(src_ref=src, dst_ref=dst, send_sem=send, recv_sem=recv,
                                            device_id=where, device_id_type=MESH)

    right, left = jnp.minimum(p + 1, n - 1), jnp.maximum(p - 1, 0)

    def right_copy(t, part):
        return remote(sr.at[t, part], gr.at[t, part], rsend.at[lax.rem(t, ring)], rrecv.at[lax.rem(t, ring)], ra=right)

    def left_copy(t, part):
        return remote(sl.at[t, part], gl.at[t, part], lsend.at[lax.rem(t, ring)], lrecv.at[lax.rem(t, ring)], ra=left)

    def hid_lanes(t):
        return pl.ds(pl.multiple_of(lax.rem(t, PAIR) * w, w), w)

    def hid_copy(t, e):
        part, k = high if e else low, lax.rem(t, hsend.shape[0])
        at = hid_lanes(t)
        return remote(hid.at[t // PAIR, part, at], hid.at[t // PAIR, part, at], hsend.at[k, e], hrecv.at[k, e],
                      ra=left if e else right)

    def square_copy(l, g, k, src):
        return remote(ss.at[l, g, src], ss.at[l, g, src], sss.at[g, k], rss.at[g, src],
                      ra=lax.rem(p + k, n))

    def send_squares(l, g):
        x = xb[l, g].astype(F32)
        col = jnp.sum(x * x, axis=1, keepdims=True)
        eye = (lax.broadcasted_iota(jnp.int32, (rows, LANES), 0)
               == lax.broadcasted_iota(jnp.int32, (rows, LANES), 1))
        row = jnp.sum(jnp.where(eye, col, 0.0), axis=0, keepdims=True)
        ss[l, g, p] = jnp.broadcast_to(row, (8, LANES))
        for k in range(1, n):
            square_copy(l, g, k, p).start()

    def take_rinv(l, g):
        for k in range(1, n):
            square_copy(l, g, k, lax.rem(p + k, n)).wait_recv()
        for k in range(1, n):
            square_copy(l, g, k, p).wait_send()
        row = ss[l, g, 0][0:1]
        for src in range(1, n):
            row = row + ss[l, g, src][0:1]
        pick = (lax.broadcasted_iota(jnp.int32, (rows, LANES), 0)
                == lax.broadcasted_iota(jnp.int32, (rows, LANES), 1))
        col = jnp.sum(jnp.where(pick, row, 0.0), axis=1, keepdims=True)
        return lax.rsqrt(col / dim + EPS)

    def scale_rows(l, g):
        scaled[g] = (xb[l, g].astype(F32) * pg[pl.ds(l, 1), :]).astype(BF16)

    for g in range(GROUPS):
        xb[0, g] = stream[g * rows:(g + 1) * rows]
        scale_rows(0, g)
    for v in range(layers * chunks):
        row, at = slice(v // chunks, v // chunks + 1), slice(v % chunks * w, (v % chunks + 1) * w)
        scales[v, 0:1, 0:w] = gs[row, at]
        scales[v, 0:1, w:2 * w] = us[row, at]

    pl.semaphore_wait(barrier, n + 1)

    for g in range(GROUPS):
        send_squares(0, g)

    def locate(u):
        s = jnp.int32(0)
        first = jnp.int32(0)
        kept = jnp.int32(ends[0])
        for k in range(1, phases):
            s = jnp.where(u >= start[k], k, s)
            first = jnp.where(u >= start[k], start[k], first)
            kept = jnp.where(u >= start[k], ends[k], kept)
        c = u - first
        return s, s // GROUPS, lax.rem(s, GROUPS), c, (u >= 0) & (c < chunks), c >= kept

    def kinds(both):
        found = [(both, True)] if min(ends) < chunks else []
        return found + ([(jnp.logical_not(both), False)] if any(ends) else [])

    def products(s, l, g, c, both):
        t, b = s * chunks + c, c // PAIR
        v = l * blocks + b

        @pl.when(g == 0)
        def _():
            k = lax.rem(v, UP_SLOTS)
            for copy in up_copies(v):
                copy.wait()

            for j in range(PAIR):
                for side in range(2):
                    at = (2 * j + side) * w
                    wub[b, :, at:at + w] = ust[k, side, :, j * w:(j + 1) * w].astype(BF16)

            @pl.when(v + UP_SLOTS < total)
            def _():
                for copy in up_copies(v + UP_SLOTS):
                    copy.start()

        @pl.when(c == 0)
        def _():
            acc[g] = jnp.zeros_like(acc[g])

        o = lax.rem(t, ring)
        sums = jnp.dot(scaled[g], wub[b], preferred_element_type=F32)
        for j in range(PAIR):
            own[o + j] = sums[:, 2 * j * w:2 * (j + 1) * w]
        for kind, whole in kinds(both):
            @pl.when(kind & (p == 0))
            def _(part=everything if whole else high):
                for j in range(PAIR):
                    sr[t + j, part] = own[o + j, part].astype(BF16)
                    right_copy(t + j, part).start()

            @pl.when(kind & (p == n - 1))
            def _(part=everything if whole else low):
                for j in range(PAIR):
                    sl[t + j, part] = own[o + j, part].astype(BF16)
                    left_copy(t + j, part).start()

    def hop(h, s, l, g, c, both):
        t = s * chunks + c
        o = lax.rem(t, ring)
        for kind, whole in kinds(both):
            @pl.when(kind & (p == h))
            def _(part=everything if whole else high):
                right_copy(t, part).wait_recv()
                sr[t, part] = (own[o, part] + gr[t, part].astype(F32)).astype(BF16)
                right_copy(t, part).start()

            @pl.when(kind & (p == n - 1 - h))
            def _(part=everything if whole else low):
                left_copy(t, part).wait_recv()
                sl[t, part] = (own[o, part] + gl[t, part].astype(F32)).astype(BF16)
                left_copy(t, part).start()

    def activate(t, v, g, o, part):
        rinv = jnp.concatenate([rinv_ref[g, part]] * (w // LANES), axis=1)
        gate = own[o, part, 0:w] * rinv * scales[v, 0:1, 0:w]
        upper = own[o, part, w:2 * w] * rinv * scales[v, 0:1, w:2 * w]
        hid[t // PAIR, part, hid_lanes(t)] = (gate / (1.0 + jnp.exp(-gate)) * upper).astype(BF16)

    def finish(s, l, g, c, both):
        t, v = s * chunks + c, l * chunks + c
        o = lax.rem(t, ring)

        @pl.when(c == 0)
        def _():
            rinv_ref[g] = jnp.broadcast_to(take_rinv(l, g), (rows, LANES))

        @pl.when(both)
        def _():
            @pl.when(p == n - 1)
            def _():
                right_copy(t, everything).wait_recv()

            @pl.when(p == 0)
            def _():
                left_copy(t, everything).wait_recv()

            @pl.when(p > 0)
            def _():
                own[o] += gr[t].astype(F32)

            @pl.when(p < n - 1)
            def _():
                own[o] += gl[t].astype(F32)

            activate(t, v, g, o, everything)

        if any(ends):
            @pl.when(jnp.logical_not(both) & (p == n - 1))
            def _():
                right_copy(t, high).wait_recv()
                own[o, high] += gr[t, high].astype(F32)
                activate(t, v, g, o, high)
                hid_copy(t, 1).start()

            @pl.when(jnp.logical_not(both) & (p == 0))
            def _():
                left_copy(t, low).wait_recv()
                own[o, low] += gl[t, low].astype(F32)
                activate(t, v, g, o, low)
                hid_copy(t, 0).start()

    def pass_on(k, s, l, g, c, both):
        t = s * chunks + c
        for e in range(2):
            @pl.when(jnp.logical_not(both) & (p == (n - 1 - k if e else k)))
            def _(e=e):
                hid_copy(t, e).wait_recv()
                if k < n - 1:
                    hid_copy(t, e).start()

    def retire(s, l, g, c, both):
        t = s * chunks + c
        for kind, whole in kinds(both):
            @pl.when(kind & (p < n - 1))
            def _(part=everything if whole else high):
                right_copy(t, part).wait_send()

            @pl.when(kind & (p > 0))
            def _(part=everything if whole else low):
                left_copy(t, part).wait_send()

    def retire_hid(s, l, g, c, both):
        t = s * chunks + c

        @pl.when(jnp.logical_not(both) & (p < n - 1))
        def _():
            hid_copy(t, 0).wait_send()

        @pl.when(jnp.logical_not(both) & (p > 0))
        def _():
            hid_copy(t, 1).wait_send()

    def take_down(l, b):
        v = l * blocks + b
        k = lax.rem(v, DOWN_SLOTS)
        down_copy(v).wait()
        wdb[b] = dst[k].astype(BF16)

        @pl.when(v + DOWN_SLOTS < total)
        def _():
            down_copy(v + DOWN_SLOTS).start()

    def down(t, g, c):
        acc[g] += jnp.dot(hid[t // PAIR], wdb[c // PAIR], preferred_element_type=F32)

    mine = pl.ds(pl.multiple_of(core * half, half), half)
    other = pl.ds(pl.multiple_of((1 - core) * half, half), half)

    def core_copy(s):
        return remote(c1s.at[s], c1r.at[s], cs.at[0, lax.rem(s, GROUPS)], cr.at[0, lax.rem(s, GROUPS)], cb=mate)

    def chip_copy(s):
        return remote(c2s.at[s], c2r.at[s], cs.at[1, lax.rem(s, GROUPS)], cr.at[1, lax.rem(s, GROUPS)], cb=xmate)

    def back_copy(s, l, g, part):
        return remote(xb.at[l + 1, g, part], xb.at[l + 1, g, part], cs.at[2, g], cr.at[2, g], cb=mate)

    def to_core(s, l, g):
        c1s[s] = acc[g, other].astype(BF16)
        core_copy(s).start()

    def to_chip(s, l, g):
        core_copy(s).wait_recv()
        c2s[s] = (acc[g, mine] + c1r[s].astype(F32)).astype(BF16)
        chip_copy(s).start()

    def to_next(s, l, g):
        chip_copy(s).wait_recv()
        branch = (c2s[s].astype(F32) + c2r[s].astype(F32)) * ds[pl.ds(l, 1), :]
        xb[l + 1, g, mine] = (0.5 * xb[l, g, mine].astype(F32) + branch).astype(BF16)
        back_copy(s, l, g, mine).start()

    def begin(s, l, g):
        back_copy(s, l, g, other).wait_recv()
        send_squares(l + 1, g)

        @pl.when(l + 1 < layers)
        def _():
            scale_rows(l + 1, g)

        core_copy(s).wait_send()
        chip_copy(s).wait_send()
        back_copy(s, l, g, mine).wait_send()

    def close(s, l, g):
        @pl.when(l + 1 == layers)
        def _():
            rinv = take_rinv(layers, g)
            at = pl.ds(pl.multiple_of(g * rows, rows), rows)
            out[at, :] = (xb[layers, g].astype(F32) * rinv * og[0:1, :]).astype(BF16)

    def at_ready(i, after, stage):
        s, hit = jnp.int32(0), jnp.bool_(False)
        for k in range(phases):
            s = jnp.where(i == ready[k] + after, k, s)
            hit = hit | (i == ready[k] + after)

        @pl.when(hit)
        def _():
            stage(s, s // GROUPS, lax.rem(s, GROUPS))

    @pl.loop(0, ready[-1] + sum(AFTER) + 1)
    def _(i):
        def run(stage, offset, every=1):
            s, l, g, c, valid, both = locate(i - offset)

            @pl.when(valid & (lax.rem(c, every) == 0) if every > 1 else valid)
            def _():
                stage(s, l, g, c, both)

        for h in range(n - 2, 0, -1):
            run(functools.partial(hop, h), h * LAG)
        run(finish, (n - 1) * LAG)
        run(retire, (n - 1) * LAG)
        if any(ends):
            for k in range(1, n):
                run(functools.partial(pass_on, k), (n - 1 + k) * LAG)

        s, l, g, c, valid, both = locate(i - (n - 1) * LAG)

        last = PAIR - 1
        full = lax.rem(c, PAIR) == last

        @pl.when(valid & full & (g == 0))
        def _():
            take_down(l, c // PAIR)

        @pl.when(valid & full & both)
        def _():
            down(s * chunks + c, g, c)

        if any(ends):
            s2, _, g2, c2, valid2, both2 = locate(i - 2 * (n - 1) * LAG)

            @pl.when(valid2 & jnp.logical_not(both2) & (lax.rem(c2, PAIR) == last))
            def _():
                down(s2 * chunks + c2, g2, c2)

        after = 0
        for stage, step in zip((to_core, to_chip, to_next, begin, close), (0,) + AFTER):
            after += step
            at_ready(i, after, stage)
        run(products, 0, PAIR)
        if any(ends):
            run(retire_hid, 2 * (n - 1) * LAG + 1)


def fused(stream, w_gate, w_up, w_down, gate_scale, up_scale, down_scale, pre_gain, out_gain):
    n = lax.axis_size("ra")
    tokens, cols = stream.shape
    layers, _, units = w_gate.shape
    chunks, rows = units // WIDTH, tokens // GROUPS
    half, phases = rows // 2, layers * GROUPS
    items = phases * chunks
    blocks, wide = chunks // PAIR, PAIR * WIDTH
    ring = -(-((n - 1) * LAG + PAIR + 1) // PAIR) * PAIR
    dma = pltpu.SemaphoreType.DMA
    scratch = [
        pltpu.VMEM((UP_SLOTS, 2, cols, wide), F32),
        pltpu.VMEM((DOWN_SLOTS, wide, cols), F32),
        pltpu.VMEM((blocks, cols, 2 * wide), BF16),
        pltpu.VMEM((blocks, wide, cols), BF16),
        dma((UP_SLOTS, 2)),
        dma((DOWN_SLOTS,)),
        pltpu.VMEM((layers + 1, GROUPS, rows, cols), BF16),
        pltpu.VMEM((GROUPS, rows, cols), BF16),
        pltpu.VMEM((ring, rows, 2 * WIDTH), F32),
    ]
    scratch += [pltpu.VMEM((items, rows, 2 * WIDTH), BF16)] * 4
    scratch += [
        pltpu.VMEM((items // PAIR, rows, wide), BF16),
        pltpu.VMEM((GROUPS, rows, cols), F32),
        pltpu.VMEM((GROUPS, rows, LANES), F32),
        pltpu.VMEM((layers * chunks, 8, 2 * WIDTH), F32),
        pltpu.VMEM((layers + 1, GROUPS, n, 8, LANES), F32),
    ]
    scratch += [pltpu.VMEM((phases, half, cols), BF16)] * 4
    scratch += [dma((ring,))] * 4
    scratch += [dma((2 * ring if any(ENDS) else 1, 2))] * 2
    scratch += [dma((GROUPS, n))] * 2
    scratch += [dma((3, GROUPS))] * 2
    vmem, hbm = pl.BlockSpec(memory_space=pltpu.VMEM), pl.BlockSpec(memory_space=pl.ANY)
    return pl.pallas_call(
        functools.partial(body, n, layers, cols * n, chunks),
        out_shape=jax.ShapeDtypeStruct((tokens, cols), BF16),
        in_specs=[vmem, hbm, hbm, hbm] + [vmem] * 5,
        out_specs=vmem,
        scratch_shapes=scratch,
        compiler_params=pltpu.CompilerParams(
            collective_id=0, has_side_effects=True, vmem_limit_bytes=64 * 1024 * 1024 - 65536
        ),
    )(stream, w_gate, w_up, w_down, gate_scale, up_scale, down_scale, pre_gain, out_gain[None])


def plain(stream, w_gate, w_up, w_down, gate_scale, up_scale, down_scale, pre_gain, out_gain):
    current = stream
    tokens = stream.shape[0]
    dim = stream.shape[1] * lax.axis_size("ra")
    share = tokens // lax.axis_size("ra")
    for layer in range(w_gate.shape[0]):
        xvals = current.astype(F32)
        squares = jnp.sum(xvals * xvals, axis=1)
        scaled = (xvals * pre_gain[layer]).astype(BF16)
        gate_part = jnp.dot(scaled, w_gate[layer].astype(BF16), preferred_element_type=F32)
        up_part = jnp.dot(scaled, w_up[layer].astype(BF16), preferred_element_type=F32)
        down_local = w_down[layer].astype(BF16)
        total = lax.psum(squares, "ra")
        summed = (
            lax.psum_scatter(gate_part, "ra", scatter_dimension=0, tiled=True),
            lax.psum_scatter(up_part, "ra", scatter_dimension=0, tiled=True),
        )
        own_rows = lax.dynamic_slice_in_dim(total, lax.axis_index("ra") * share, share)
        rinv = lax.rsqrt(own_rows / dim + EPS)[:, None]
        gate = summed[0] * rinv * gate_scale[layer]
        upper = summed[1] * rinv * up_scale[layer]
        hidden = (jax.nn.silu(gate) * upper).astype(BF16)
        terms = jnp.dot(
            lax.all_gather(hidden, "ra", axis=0, tiled=True), down_local, preferred_element_type=F32
        )
        branch = lax.psum(terms.astype(BF16), "cb").astype(F32) * down_scale[layer]
        current = (0.5 * xvals + branch).astype(BF16)
    xvals = current.astype(F32)
    final_sum = lax.psum(jnp.sum(xvals * xvals, axis=1), "ra")
    rinv = lax.rsqrt(final_sum / dim + EPS)[:, None]
    return (xvals * rinv * out_gain).astype(BF16)


def local(*args):
    n = lax.axis_size("ra")
    tokens, cols = args[0].shape
    fits = (n >= 2 and tokens == 128 and n <= 8 and lax.axis_size("cb") == 4
            and args[1].shape[2] % (PAIR * WIDTH) == 0 and cols % LANES == 0)
    return (fused if fits else plain)(*args)


def solution(mesh):
    placed = (
        P("grp", "ra"),
        P(None, "ra", "cb"),
        P(None, "ra", "cb"),
        P(None, "cb", "ra"),
        P(None, "cb"),
        P(None, "cb"),
        P(None, "ra"),
        P(None, "ra"),
        P("ra"),
    )
    return jax.shard_map(
        local, mesh=mesh, in_specs=placed, out_specs=P("grp", "ra"), check_vma=False
    )
```
